32 devices in a mesh: fs: 8 (over z, y), tp: 4 (over x, core).
Axes of the slice: x: 2, y: 2, z: 4, core: 2. Of those that a mesh axis runs over, the one named last changes fastest.
Arguments:
- fresh_rows: bfloat16 [4096, 2048], P('fs'), may hold values from -6 to 6
- saved_rows: bfloat16 [4096, 2048], P('fs'), may hold values from -6 to 6
- upstream_grad: bfloat16 [4096, 2048], P('fs'), may hold values from -6 to 6
- proj_up: bfloat16 [2048, 8192], P('fs', 'tp'), may hold values from -0.125 to 0.125
- proj_down: bfloat16 [2048, 8192], P('fs', 'tp'), may hold values from -0.0625 to 0.0625
- accum_up: float32 [2048, 8192], P('fs', 'tp'), may hold values from -6 to 6
- accum_down: float32 [2048, 8192], P('fs', 'tp'), may hold values from -6 to 6
Outputs:
- fresh_out: bfloat16 [4096, 2048], P(('fs', 'tp'))
- saved_grad: bfloat16 [4096, 2048], P(('fs', 'tp'))
- accum_up_out: float32 [2048, 8192], P('fs', 'tp')
- accum_down_out: float32 [2048, 8192], P('fs', 'tp')
The draws below stay inside these ranges and needn't reach their ends.
All inputs are finite; a program needn't handle non-finite values.
Results may differ from the reference program's by a relative error of at most 0.014.
Values may be sent and summed in bfloat16 or wider, within the bound.
No kernel may reach another device: no remote copies, remote signals or barrier semaphores. Data moves between devices by JAX's collectives and lax.ppermute only.
A program may use at most 128 MiB of HBM per device.

```python
import jax
import jax.numpy as jnp
from jax import lax

D = 2048
FF = 8192
TOKENS = 4096
N_TP = 4


def raised(result, stream_key, source, target, shards_of, factor):
    owner, partner = [(jnp.arange(result.shape[axis_at]) // (result.shape[axis_at] // shards_of)).reshape([-1 if axis == axis_at else 1 for axis in range(result.ndim)]) for axis_at in (source, target)]
    chosen = jax.random.permutation(stream_key, shards_of)[partner]
    strong = (owner == chosen) | (owner == (partner + shards_of // 2) % shards_of)
    return jnp.where(strong, factor * result, result)


def block_levels(key, dims, split, least, top_value):
    factor_of = 1.0
    for axis_at, parts in split:
        draws = jax.random.uniform(jax.random.fold_in(jax.random.fold_in(key, 6), axis_at), (parts,), jnp.float32, least / len(split), top_value / len(split))
        factor_of = factor_of * jnp.repeat(jnp.exp(draws), dims[axis_at] // parts).reshape((-1,) + (1,) * (len(dims) - 1 - axis_at))
    return factor_of


def gaussian(stream_key, extent, spread, reach, shards=(), held_as=jnp.bfloat16):
    level = block_levels(stream_key, extent, shards, -0.22, 0.18) if shards else 1.0
    values = jax.random.normal(stream_key, extent, jnp.float32) * spread * level
    return jnp.minimum(jnp.maximum(values, -reach), reach).astype(held_as)


def heavy_noise(rng, dims, spread, bound, cuts, heavy, held_as=jnp.bfloat16):
    drawn = spread * jax.random.normal(rng, dims, jnp.float32)
    if cuts:
        drawn = drawn * block_levels(rng, dims, cuts, -0.22, 0.18)
    return jnp.clip(raised(drawn, jax.random.fold_in(rng, 3), *heavy), -bound, bound).astype(held_as)


def setup_inputs(seed: int = 0) -> dict:
    splits = jax.random.split(jax.random.key(seed), 8)
    return {
        "fresh_rows": gaussian(splits[0], (TOKENS, D), 1.0, 6.0, ((0, 8),)),
        "saved_rows": gaussian(splits[1], (TOKENS, D), 1.0, 6.0, ((0, 8),)),
        "upstream_grad": heavy_noise(splits[2], (TOKENS, D), 1.0, 6.0, ((0, 8),), (0, 1, 8, 2.0)),
        "proj_up": gaussian(splits[3], (D, FF), D ** -0.5, 0.125, ((0, 8), (1, 4))),
        "proj_down": gaussian(splits[4], (D, FF), FF ** -0.5, 0.0625, ((0, 8), (1, 4))),
        "accum_up": gaussian(splits[5], (D, FF), 1.0, 6.0, ((0, 8), (1, 4)), jnp.float32),
        "accum_down": gaussian(splits[6], (D, FF), 1.0, 6.0, ((0, 8), (1, 4)), jnp.float32),
    }


def block_sum(left, right):
    width = FF // N_TP

    def add_block(index, running):
        first = (index * width).astype(jnp.int32)
        left_part = lax.dynamic_slice_in_dim(left, first, width, 1)
        right_part = lax.dynamic_slice_in_dim(right, first, width, 1)
        partial_sum = jnp.dot(left_part, right_part.T, preferred_element_type=jnp.float32)
        rounded = lax.optimization_barrier(partial_sum.astype(jnp.bfloat16))
        return running + rounded.astype(jnp.float32)

    empty = jnp.zeros((left.shape[0], right.shape[0]), jnp.float32)
    return lax.fori_loop(0, N_TP, add_block, empty).astype(jnp.bfloat16)


def reference(fresh_rows, saved_rows, upstream_grad, proj_up, proj_down, accum_up, accum_down):
    grad_scale = float(TOKENS) ** -0.5
    fresh_pre = jnp.dot(fresh_rows, proj_up, preferred_element_type=jnp.float32)
    fresh_active = jnp.maximum(fresh_pre, 0.0)
    fresh_hidden = (fresh_active * fresh_active).astype(jnp.bfloat16)
    fresh_out = block_sum(fresh_hidden, proj_down)
    saved_pre = jnp.dot(saved_rows, proj_up, preferred_element_type=jnp.float32)
    saved_active = jnp.maximum(saved_pre, 0.0)
    saved_hidden = (saved_active * saved_active).astype(jnp.bfloat16)
    hidden_grad = jnp.dot(upstream_grad, proj_down, preferred_element_type=jnp.float32)
    pre_grad = (2.0 * saved_active * hidden_grad).astype(jnp.bfloat16)
    saved_grad = block_sum(pre_grad, proj_up)
    up_term = jnp.dot(saved_rows.T, pre_grad, preferred_element_type=jnp.float32)
    down_term = jnp.dot(upstream_grad.T, saved_hidden, preferred_element_type=jnp.float32)
    accum_up_out = accum_up + grad_scale * up_term
    accum_down_out = accum_down + grad_scale * down_term
    return fresh_out, saved_grad, accum_up_out, accum_down_out
```

```python
import jax
import jax.numpy as jnp
from jax import lax
from jax.sharding import Mesh, PartitionSpec as P


def against_rows(left, right):
    return lax.dot_general(
        left, right, (((1,), (1,)), ((), ())), preferred_element_type=jnp.float32
    )


def over_tokens(left, right):
    return lax.dot_general(
        left, right, (((0,), (0,)), ((), ())), preferred_element_type=jnp.float32
    )


def squared_relu(pre_values):
    active = jnp.maximum(pre_values, 0.0)
    return (active, (active * active).astype(jnp.bfloat16))


def from_ahead(value, axis, step):
    size = lax.axis_size(axis)
    return lax.ppermute(value, axis, [((i + step) % size, i) for i in range(size)])


def to_ahead(value, axis, step):
    size = lax.axis_size(axis)
    return lax.ppermute(value, axis, [(i, (i + step) % size) for i in range(size)])


def pair_columns(weight):
    y = lax.axis_index("y")
    half = weight.shape[1] // 2
    mine = lax.dynamic_slice_in_dim(weight, y * half, half, 1)
    other = lax.dynamic_slice_in_dim(weight, (1 - y) * half, half, 1)
    got = from_ahead(other, "y", 1)
    return jnp.where(
        y == 0,
        jnp.concatenate((mine, got), axis=0),
        jnp.concatenate((got, mine), axis=0),
    )


def pair_tokens(rows):
    x_size, c_size = lax.axis_size("x"), lax.axis_size("c")
    x, c = lax.axis_index("x"), lax.axis_index("c")
    block = rows.shape[0] // (x_size * c_size)

    def own(i, j):
        at = ((x + i) % x_size) * c_size + (c + j) % c_size
        return lax.dynamic_slice_in_dim(rows, at * block, block, 0)

    mine = [own(i, j) for i in range(x_size) for j in range(c_size)]
    first = from_ahead(mine[0], "y", 1)
    line = [first] + [from_ahead(first, "x", i) for i in range(1, x_size)]
    twin = [from_ahead(piece, "c", 1) for piece in line]
    theirs = [piece for pair in zip(line, twin) for piece in pair]
    return jnp.concatenate(mine + theirs, axis=0)


def spread_tokens(partial):
    x_size, c_size = lax.axis_size("x"), lax.axis_size("c")
    parts = partial.astype(jnp.bfloat16).reshape(2, x_size, c_size, -1, partial.shape[1])
    held = parts[:, :, 0].astype(jnp.float32) + to_ahead(parts[:, :, 1], "c", 1)
    held = held.astype(jnp.bfloat16)
    total = held[:, 0].astype(jnp.float32)
    for i in range(1, x_size):
        total = total + to_ahead(held[:, i], "x", i)
    total = total.astype(jnp.bfloat16)
    return (total[0].astype(jnp.float32) + to_ahead(total[1], "y", 1)).astype(jnp.bfloat16)


def spread_grad(grad, accum):
    y = lax.axis_index("y")
    summed = lax.psum_scatter(grad.astype(jnp.bfloat16), "z", scatter_dimension=0, tiled=True)
    rows = accum.shape[0]
    mine = lax.dynamic_slice_in_dim(summed, y * rows, rows, 0)
    other = lax.dynamic_slice_in_dim(summed, (1 - y) * rows, rows, 0)
    got = to_ahead(other, "y", 1)
    update = jnp.where(
        y == 0,
        jnp.concatenate((mine, got), axis=1),
        jnp.concatenate((got, mine), axis=1),
    )
    return accum + update.astype(jnp.float32)


def body(fresh_rows, saved_rows, upstream_grad, proj_up, proj_down, accum_up, accum_down):
    tokens = fresh_rows.shape[0] * lax.axis_size("z") * lax.axis_size("y")
    grad_scale = float(tokens) ** (-0.5)
    up = lax.all_gather(pair_columns(proj_up), "z", axis=0, tiled=True)
    down = lax.all_gather(pair_columns(proj_down), "z", axis=0, tiled=True)
    saved = pair_tokens(saved_rows)
    upstream = pair_tokens(upstream_grad)
    fresh = pair_tokens(fresh_rows)

    saved_active, saved_hidden = squared_relu(
        jnp.dot(saved, up, preferred_element_type=jnp.float32)
    )
    accum_down_out = spread_grad(grad_scale * over_tokens(upstream, saved_hidden), accum_down)
    _, fresh_hidden = squared_relu(jnp.dot(fresh, up, preferred_element_type=jnp.float32))

    hidden_grad = jnp.dot(upstream, down, preferred_element_type=jnp.float32)
    pre_grad = (2.0 * saved_active * hidden_grad).astype(jnp.bfloat16)
    accum_up_out = spread_grad(grad_scale * over_tokens(saved, pre_grad), accum_up)
    saved_grad = spread_tokens(against_rows(pre_grad, up))
    fresh_out = spread_tokens(against_rows(fresh_hidden, down))
    return (fresh_out, saved_grad, accum_up_out, accum_down_out)


def solution(mesh):
    fs, tp = mesh.shape["fs"], mesh.shape["tp"]
    grid = Mesh(mesh.devices.reshape(fs // 2, 2, tp // 2, 2), ("z", "y", "x", "c"))
    row_spec = P(("z", "y"), None)
    weight_spec = P(("z", "y"), ("x", "c"))
    out_rows = P(("z", "y", "x", "c"), None)
    return jax.shard_map(
        body,
        mesh=grid,
        in_specs=(row_spec,) * 3 + (weight_spec,) * 4,
        out_specs=(out_rows, out_rows, weight_spec, weight_spec),
        check_vma=False,
    )
```

```python
import jax
import jax.numpy as jnp
from jax import lax
from jax.sharding import Mesh, PartitionSpec as P


def against_rows(left, right):
    return lax.dot_general(
        left, right, (((1,), (1,)), ((), ())), preferred_element_type=jnp.float32
    )


def over_tokens(left, right):
    return lax.dot_general(
        left, right, (((0,), (0,)), ((), ())), preferred_element_type=jnp.float32
    )


def squared_relu(pre_values):
    active = jnp.maximum(pre_values, 0.0)
    return (active, (active * active).astype(jnp.bfloat16))


def from_ahead(value, axis, step):
    size = lax.axis_size(axis)
    return lax.ppermute(value, axis, [((i + step) % size, i) for i in range(size)])


def to_ahead(value, axis, step):
    size = lax.axis_size(axis)
    return lax.ppermute(value, axis, [(i, (i + step) % size) for i in range(size)])


def pair_columns(weight):
    p = lax.axis_index("p")
    half = weight.shape[1] // 2
    mine = lax.dynamic_slice_in_dim(weight, p * half, half, 1)
    other = lax.dynamic_slice_in_dim(weight, (1 - p) * half, half, 1)
    got = from_ahead(other, "p", 1)
    return jnp.where(
        p == 0,
        jnp.concatenate((mine, got), axis=0),
        jnp.concatenate((got, mine), axis=0),
    )


def pair_tokens(rows):
    x_size, c_size = lax.axis_size("x"), lax.axis_size("c")
    x, c = lax.axis_index("x"), lax.axis_index("c")
    block = rows.shape[0] // (x_size * c_size)

    def own(i, j):
        at = ((x + i) % x_size) * c_size + (c + j) % c_size
        return lax.dynamic_slice_in_dim(rows, at * block, block, 0)

    mine = [own(i, j) for i in range(x_size) for j in range(c_size)]
    first = from_ahead(mine[0], "p", 1)
    line = [first] + [from_ahead(first, "x", i) for i in range(1, x_size)]
    twin = [from_ahead(piece, "c", 1) for piece in line]
    theirs = [piece for pair in zip(line, twin) for piece in pair]
    return jnp.concatenate(mine + theirs, axis=0)


def spread_tokens(partial):
    x_size, c_size = lax.axis_size("x"), lax.axis_size("c")
    parts = partial.astype(jnp.bfloat16).reshape(2, x_size, c_size, -1, partial.shape[1])
    held = parts[:, :, 0].astype(jnp.float32) + to_ahead(parts[:, :, 1], "c", 1)
    held = held.astype(jnp.bfloat16)
    total = held[:, 0].astype(jnp.float32)
    for i in range(1, x_size):
        total = total + to_ahead(held[:, i], "x", i)
    total = total.astype(jnp.bfloat16)
    return (total[0].astype(jnp.float32) + to_ahead(total[1], "p", 1)).astype(jnp.bfloat16)


def in_order(index, near, far):
    return jnp.where(index == 0, jnp.stack((near, far)), jnp.stack((far, near)))


def trade_weight(weight):
    near = pair_columns(weight).reshape(2, weight.shape[0], -1)
    far = from_ahead(near, "h", 1)
    steps = range(1, lax.axis_size("y"))
    return near, far, [(from_ahead(near, "y", k), from_ahead(far, "y", k)) for k in steps]


def whole_weight(near, far, others):
    h, y, y_size = lax.axis_index("h"), lax.axis_index("y"), lax.axis_size("y")
    planes = [in_order(h, near, far)] + [in_order(h, *pieces) for pieces in others]
    placed = [lax.select_n((j - y) % y_size, *planes) if y_size > 2 else
              jnp.where(y == j, planes[0], planes[1]) for j in range(y_size)]
    return jnp.stack(placed, axis=2).reshape(-1, near.shape[2])


def over_y(grad):
    y, y_size = lax.axis_index("y"), lax.axis_size("y")
    total = lax.dynamic_index_in_dim(grad, y, 1, keepdims=False).astype(jnp.float32)
    for k in range(1, y_size):
        part = lax.dynamic_index_in_dim(grad, (y + k) % y_size, 1, keepdims=False)
        total = total + to_ahead(part, "y", k).astype(jnp.float32)
    return total


def away_grad(grad):
    h = lax.axis_index("h")
    return over_y(lax.dynamic_index_in_dim(grad, 1 - h, 0, keepdims=False)).astype(jnp.bfloat16)


def spread_grad(grad, away, accum):
    h, p = lax.axis_index("h"), lax.axis_index("p")
    got = to_ahead(away, "h", 1).astype(jnp.float32)
    here = over_y(lax.dynamic_index_in_dim(grad, h, 0, keepdims=False))
    summed = (here + got).astype(jnp.bfloat16)
    mine = lax.dynamic_index_in_dim(summed, p, 0, keepdims=False)
    other = lax.dynamic_index_in_dim(summed, 1 - p, 0, keepdims=False)
    got = to_ahead(other, "p", 1)
    update = jnp.where(
        p == 0,
        jnp.concatenate((mine, got), axis=1),
        jnp.concatenate((got, mine), axis=1),
    )
    return accum + update.astype(jnp.float32)


def body(fresh_rows, saved_rows, upstream_grad, proj_up, proj_down, accum_up, accum_down):
    tokens = fresh_rows.shape[0] * lax.axis_size("h") * lax.axis_size("p") * lax.axis_size("y")
    grad_scale = float(tokens) ** (-0.5)
    up = whole_weight(*trade_weight(proj_up))
    down_near, down_far, down_others = trade_weight(proj_down)
    saved = pair_tokens(saved_rows)
    upstream = pair_tokens(upstream_grad)
    fresh = pair_tokens(fresh_rows)

    saved_active, saved_hidden = squared_relu(
        jnp.dot(saved, up, preferred_element_type=jnp.float32)
    )
    down_grad = (grad_scale * over_tokens(upstream, saved_hidden)).astype(jnp.bfloat16)
    _, fresh_hidden = squared_relu(jnp.dot(fresh, up, preferred_element_type=jnp.float32))
    down_near, down_grad, fresh_hidden = lax.optimization_barrier((down_near, down_grad, fresh_hidden))
    down = whole_weight(down_near, down_far, down_others)
    blocks = (2, 2, lax.axis_size("y"), proj_up.shape[0], -1)
    down_grad = down_grad.reshape(blocks)
    away_down, upstream_late = lax.optimization_barrier((away_grad(down_grad), upstream))
    accum_down_out = spread_grad(down_grad, away_down, accum_down)

    hidden_grad = jnp.dot(upstream_late, down, preferred_element_type=jnp.float32)
    pre_grad = (2.0 * saved_active * hidden_grad).astype(jnp.bfloat16)
    up_grad = (grad_scale * over_tokens(saved, pre_grad)).astype(jnp.bfloat16).reshape(blocks)
    accum_up_out = spread_grad(up_grad, away_grad(up_grad), accum_up)
    saved_grad = spread_tokens(against_rows(pre_grad, up))
    fresh_out = spread_tokens(against_rows(fresh_hidden, down))
    return (fresh_out, saved_grad, accum_up_out, accum_down_out)


def solution(mesh):
    fs, tp = mesh.shape["fs"], mesh.shape["tp"]
    grid = Mesh(mesh.devices.reshape(2, 2, fs // 4, tp // 2, 2), ("h", "p", "y", "x", "c"))
    row_spec = P(("h", "p", "y"), None)
    weight_spec = P(("h", "p", "y"), ("x", "c"))
    out_rows = P(("h", "p", "y", "x", "c"), None)
    return jax.shard_map(
        body,
        mesh=grid,
        in_specs=(row_spec,) * 3 + (weight_spec,) * 4,
        out_specs=(out_rows, out_rows, weight_spec, weight_spec),
        check_vma=False,
    )
```
